32 devices in a mesh: ep: 8 (over z, x), tp: 4 (over y, core).
Axes of the slice: x: 2, y: 2, z: 4, core: 2. Of those that a mesh axis runs over, the one named last changes fastest.
Arguments:
- tokens: bfloat16 [192, 2048], P('ep'), may hold values from -12 to 12
- state: float32 [192, 16, 128, 256], P('ep', 'tp'), may hold values from -6 to 6
- w_query: bfloat16 [2048, 2048], P(None, 'tp'), may hold values from -0.125 to 0.125
- w_key: bfloat16 [2048, 2048], P(None, 'tp'), may hold values from -0.125 to 0.125
- w_value: bfloat16 [2048, 4096], P(None, 'tp'), may hold values from -0.125 to 0.125
- w_outgate: bfloat16 [2048, 4096], P(None, 'tp'), may hold values from -0.125 to 0.125
- decay_down: bfloat16 [2048, 16], replicated, may hold values from -0.125 to 0.125
- decay_up: bfloat16 [16, 2048], P(None, 'tp'), may hold values from -9 to 9
- decay_bias: float32 [2048], P('tp'), may hold values from -6 to 4
- head_gain: float32 [256], replicated, may hold values from 0.1 to 1.9
- w_output: bfloat16 [4096, 2048], P('tp'), may hold values from -0.09375 to 0.09375
- norm1_gain: float32 [2048], P('tp'), may hold values from 0.1 to 1.9
- route_ids: int32 [192, 6], P('ep'), may hold values from 0 to 31, all different within a row; in each aligned block of 24 rows (0 to 23, 24 to 47, ...) at most 5 rows name the same one
- route_weight: float32 [192, 6], P('ep'), may hold values from 0.1 to 1
- exp_gate: bfloat16 [32, 2048, 512], P('ep', 'tp'), may hold values from -0.125 to 0.125
- exp_up: bfloat16 [32, 2048, 512], P('ep', 'tp'), may hold values from -0.125 to 0.125
- exp_down: bfloat16 [32, 512, 2048], P('ep', None, 'tp'), may hold values from -0.25 to 0.25
- sh_gate: bfloat16 [2048, 512], P('tp'), may hold values from -0.125 to 0.125
- sh_up: bfloat16 [2048, 512], P('tp'), may hold values from -0.125 to 0.125
- sh_down: bfloat16 [512, 2048], P(None, 'tp'), may hold values from -0.25 to 0.25
- norm2_gain: float32 [2048], P('tp'), may hold values from 0.1 to 1.9
Outputs:
- layer_out: bfloat16 [192, 2048], P('ep', 'tp')
The draws below stay inside these ranges and needn't reach their ends.
Inputs may be any that keep to these rules, and one draw needn't show every extreme that they name: `route_ids`: each row names 6 different experts. Among the rows of one index of ep (aligned blocks of 24 rows) no expert is named by more than 5 rows, and in some blocks one expert is named by exactly 5.
All inputs are finite; a program needn't handle non-finite values.
Results may differ from the reference program's by a relative error of at most 0.02.
Values may be sent and summed in bfloat16 or wider, within the bound.
A program may use at most 64 MiB of HBM per device.

```python
import math
import jax
import jax.numpy as jnp
import numpy as np
from jax import lax

D = 2048
HEADS = 16
KEY_DIM = 128
VAL_DIM = 256
RANK = 16
FF_EXP = 512
FF_SHARED = 512
TOPK = 6
TOK_DEV = 24
BATCH = 192
EXPERTS = 32
CAP = 5
N_EP = 8
N_TP = 4


def draw_tokens(key, part):
    column = jnp.arange(D, dtype=jnp.float32) / D
    ramp = jnp.exp((2.0 * column - 1.0) * jnp.log(3.0))
    drawn = jax.random.normal(key, (BATCH, D), jnp.float32) * ramp
    return jnp.clip(drawn, -12.0, 12.0).astype(jnp.bfloat16)


def block_scale(stream_key, dims, cuts, smallest, top_value):
    loudness, own = 1.0, jax.random.fold_in(stream_key, 6)
    for axis_at, shards_of in cuts:
        heights = jnp.exp(jax.random.uniform(jax.random.fold_in(own, axis_at), (shards_of,), jnp.float32, smallest / len(cuts), top_value / len(cuts)))
        loudness = loudness * jnp.repeat(heights, dims[axis_at] // shards_of).reshape([-1 if axis == axis_at else 1 for axis in range(len(dims))])
    return loudness


def assign_block(rng, own, number, rows, number_of, top, limit, lean):
    sequence = jax.random.permutation(rng, number_of)
    heavy_load, common = load_shares(number_of, rows * top, limit, lean, True), load_shares(number_of, rows * top, limit, lean, False)
    places = jnp.arange(number_of)

    def named(lengths, turn):
        used = int((lengths > 0).sum())
        fixed = max(1, used // 4)
        moved = fixed + (places - fixed + turn * (used - fixed)) % max(1, number_of - fixed)
        return jnp.zeros((number_of,), jnp.int32).at[sequence[jnp.where(places < fixed, places, moved)]].set(jnp.asarray(lengths, jnp.int32))

    lengths = jnp.where(number % 4 == 0, named(heavy_load, number // 4), named(common, number - number // 4 - 1))
    mixed = jax.random.permutation(jax.random.fold_in(own, 3), number_of)
    giver, sink = mixed[0:number_of // 2 * 2:2], mixed[1:number_of // 2 * 2:2]
    margin = jnp.minimum(lengths[giver] - 1, limit - lengths[sink]) // 2
    margin = jnp.where((giver == sequence[0]) | (sink == sequence[0]) | (lengths[sink] == 0), 0, jnp.maximum(margin, 0))
    moved = jax.random.randint(jax.random.fold_in(own, 4), (number_of // 2,), 0, 1 << 20) % (margin + 1)
    lengths = lengths.at[giver].add(-moved).at[sink].add(moved)
    members = jnp.searchsorted(jnp.cumsum(lengths), jnp.arange(rows * top), side="right").astype(jnp.int32)
    listing = members.reshape(top, rows).T
    listing = listing[jax.random.permutation(jax.random.fold_in(own, 1), rows)]
    turn = jax.random.randint(jax.random.fold_in(own, 2), (rows, 1), 0, top)
    return jnp.take_along_axis(listing, (jnp.arange(top)[None, :] + turn) % top, axis=1)


def load_shares(count, total, reach, skew, full):
    weights = [(1 << 20) // math.isqrt(grade ** skew) + 1 for grade in range(1, count + 1)]
    largest = reach if full else min(reach, max(-(-total // count), total * weights[0] // sum(weights)))
    least = 1 if total - largest >= count - 1 else 0
    holding, spare = [largest] + [least] * (count - 1), total - largest - least * (count - 1)
    while spare > 0:
        movable = [i for i in range(1, count) if holding[i] < largest] or [i for i in range(1, count) if holding[i] < reach]
        whole, remaining = sum([weights[i] for i in movable]), spare
        for i in movable:
            more = min(reach - holding[i], max(1, remaining * weights[i] // whole), spare)
            holding[i] = holding[i] + more
            spare = spare - more
    return np.array(holding)


def noise(stream_key, extent, scale, limit, cuts=(), kind=jnp.bfloat16):
    loudness = block_scale(stream_key, extent, cuts, -0.22, 0.18) if cuts else 1.0
    values = jax.random.normal(stream_key, extent, jnp.float32) * scale * loudness
    return jnp.minimum(jnp.maximum(values, -limit), limit).astype(kind)


def setup_inputs(seed: int = 0) -> dict:
    keys = jax.random.split(jax.random.key(seed), 22)
    tokens = draw_tokens(jax.random.fold_in(keys[21], 71), 0)
    state = noise(keys[1], (BATCH, HEADS, KEY_DIM, VAL_DIM), 1.0, 6.0, ((0, 8), (1, 4)), jnp.float32)
    w_query = noise(keys[2], (D, HEADS * KEY_DIM), D ** -0.5, 0.125, ((1, 4),))
    w_key = noise(keys[3], (D, HEADS * KEY_DIM), D ** -0.5, 0.125, ((1, 4),))
    w_value = noise(keys[4], (D, HEADS * VAL_DIM), D ** -0.5, 0.125, ((1, 4),))
    w_outgate = noise(keys[5], (D, HEADS * VAL_DIM), D ** -0.5, 0.125, ((1, 4),))
    decay_down = noise(keys[6], (D, RANK), D ** -0.5, 0.125)
    decay_up = noise(keys[7], (RANK, HEADS * KEY_DIM), 1.5, 9.0, ((1, 4),))
    decay_bias = jnp.clip(-6.0 + 10.0 * jax.random.uniform(keys[8], (HEADS * KEY_DIM,), jnp.float32) ** block_scale(keys[8], (HEADS * KEY_DIM,), ((0, 4),), -0.2, 0.2), -6.0, 4.0)
    head_gain = jnp.clip(1.0 + 0.18 * jax.random.normal(keys[9], (VAL_DIM,), jnp.float32), 0.1, 1.9)
    w_output = noise(keys[10], (HEADS * VAL_DIM, D), (HEADS * VAL_DIM) ** -0.5, 0.09375, ((0, 4),))
    norm1_gain = jnp.clip(1.0 + 0.18 * jax.random.normal(keys[11], (D,), jnp.float32), 0.1, 1.9)
    route_ids_keys = jax.random.split(jax.random.fold_in(keys[12], 1), BATCH // TOK_DEV)
    route_ids_turns = jax.random.permutation(jax.random.fold_in(keys[12], 3), BATCH // TOK_DEV)
    route_ids = jax.vmap(lambda own, number: assign_block(jax.random.fold_in(keys[12], 2), own, number, TOK_DEV, EXPERTS, TOPK, CAP, 2))(route_ids_keys, route_ids_turns).reshape((BATCH, TOPK))
    route_weight = jnp.clip(0.1 + 0.9 * jax.random.uniform(keys[13], (BATCH, TOPK), jnp.float32) ** block_scale(keys[13], (BATCH, TOPK), ((0, 8),), -0.2, 0.2), 0.1, 1.0)
    exp_gate = noise(keys[14], (EXPERTS, D, FF_EXP), D ** -0.5, 0.125, ((0, 8), (1, 4)))
    exp_up = noise(keys[15], (EXPERTS, D, FF_EXP), D ** -0.5, 0.125, ((0, 8), (1, 4)))
    exp_down = noise(keys[16], (EXPERTS, FF_EXP, D), FF_EXP ** -0.5, 0.25, ((0, 8), (2, 4)))
    sh_gate = noise(keys[17], (D, FF_SHARED), D ** -0.5, 0.125, ((0, 4),))
    sh_up = noise(keys[18], (D, FF_SHARED), D ** -0.5, 0.125, ((0, 4),))
    sh_down = noise(keys[19], (FF_SHARED, D), FF_SHARED ** -0.5, 0.25, ((1, 4),))
    norm2_gain = jnp.clip(1.0 + 0.18 * jax.random.normal(keys[20], (D,), jnp.float32), 0.1, 1.9)
    return dict(tokens=tokens, state=state, w_query=w_query, w_key=w_key, w_value=w_value, w_outgate=w_outgate, decay_down=decay_down, decay_up=decay_up, decay_bias=decay_bias, head_gain=head_gain, w_output=w_output, norm1_gain=norm1_gain, route_ids=route_ids, route_weight=route_weight, exp_gate=exp_gate, exp_up=exp_up, exp_down=exp_down, sh_gate=sh_gate, sh_up=sh_up, sh_down=sh_down, norm2_gain=norm2_gain)


res_scale = 2.0 ** 0.5
decay_tau = 16.0
norm_eps = 1e-05

def settle(values):
    return lax.optimization_barrier(values.astype(jnp.bfloat16)).astype(jnp.float32)

def project(left, right):
    return jnp.dot(left, right, preferred_element_type=jnp.float32)

def grouped_sum(left, right, group_count):
    width = right.shape[0] // group_count

    def add_group(running, group_index):
        left_piece = lax.dynamic_slice_in_dim(left, group_index * width, width, 1)
        right_block = lax.dynamic_slice_in_dim(right, group_index * width, width, 0)
        return (running + settle(project(left_piece, right_block)), None)
    start = jnp.zeros((left.shape[0], right.shape[1]), jnp.float32)
    running, _ = lax.scan(add_group, start, jnp.arange(group_count, dtype=jnp.int32))
    return running

def layer_norm(values, gain):
    center = values - lax.optimization_barrier(jnp.mean(values, -1, keepdims=True))
    spread = lax.optimization_barrier(jnp.mean(center * center, -1, keepdims=True))
    return center * lax.rsqrt(spread + norm_eps) * gain

def reference(tokens, state, w_query, w_key, w_value, w_outgate, decay_down, decay_up, decay_bias, head_gain, w_output, norm1_gain, route_ids, route_weight, exp_gate, exp_up, exp_down, sh_gate, sh_up, sh_down, norm2_gain):
    queries = settle(project(tokens, w_query)).reshape(BATCH, HEADS, KEY_DIM) * KEY_DIM ** (-0.5)
    key_rows = settle(project(tokens, w_key)).reshape(BATCH, HEADS, KEY_DIM)
    values = settle(project(tokens, w_value)).reshape(BATCH, HEADS, VAL_DIM)
    gate_pre = settle(project(tokens, w_outgate)).reshape(BATCH, HEADS, VAL_DIM)
    decay_low = lax.optimization_barrier(project(tokens, decay_down).astype(jnp.bfloat16))
    log_decay = (jax.nn.log_sigmoid(project(decay_low, decay_up) + decay_bias) / decay_tau).reshape(BATCH, HEADS, KEY_DIM)
    carried = jnp.einsum('bhk,bhkv->bhv', queries * jnp.exp(log_decay), state, precision=lax.Precision.HIGHEST)
    attended = carried + lax.optimization_barrier(jnp.sum(queries * key_rows, -1, keepdims=True)) * values
    inv_norm = lax.rsqrt(lax.optimization_barrier(jnp.mean(attended * attended, -1, keepdims=True)) + norm_eps)
    head_out = (attended * inv_norm * head_gain * jax.nn.silu(gate_pre)).astype(jnp.bfloat16).reshape(BATCH, HEADS * VAL_DIM)
    mixed = settle(grouped_sum(head_out, w_output, N_TP))
    normed_mid = layer_norm(res_scale * tokens.astype(jnp.float32) + mixed, norm1_gain)
    normed_mid = lax.optimization_barrier(normed_mid.astype(jnp.bfloat16))
    pair_count = TOK_DEV * TOPK
    expert_ids = route_ids.reshape(N_EP, pair_count)
    onehot = (expert_ids[:, :, None] == jnp.arange(EXPERTS, dtype=jnp.int32)[None, None, :]).astype(jnp.int32)
    ranks = lax.optimization_barrier(jnp.sum((jnp.cumsum(onehot, 1) - 1) * onehot, -1))
    group_ids = jnp.arange(N_EP, dtype=jnp.int32)[:, None]
    positions = (expert_ids * (N_EP * CAP) + group_ids * CAP + ranks).reshape(BATCH * TOPK)
    token_ids = jnp.arange(BATCH * TOPK, dtype=jnp.int32) // TOPK
    table = jnp.full((EXPERTS * N_EP * CAP,), BATCH, jnp.int32).at[positions].set(token_ids)
    padded = jnp.concatenate([normed_mid, jnp.zeros((1, D), jnp.bfloat16)], 0)

    def one_expert(operands):
        row_ids, gate_weight, up_weight, down_weight = operands
        chosen = padded[row_ids]
        gate_sum = settle(grouped_sum(chosen, gate_weight, N_TP))
        up_sum = settle(grouped_sum(chosen, up_weight, N_TP))
        inner = (jax.nn.silu(gate_sum) * up_sum).astype(jnp.bfloat16)
        return project(inner, down_weight).astype(jnp.bfloat16)
    expert_out = lax.map(one_expert, (table.reshape(EXPERTS, N_EP * CAP), exp_gate, exp_up, exp_down))
    expert_out = expert_out.reshape(EXPERTS * N_EP * CAP, D)
    picked = expert_out[positions].astype(jnp.float32).reshape(BATCH, TOPK, D)
    routed = lax.optimization_barrier(jnp.sum(picked * route_weight[:, :, None], 1))
    shared_gate = settle(grouped_sum(normed_mid, sh_gate, N_TP))
    shared_up = settle(grouped_sum(normed_mid, sh_up, N_TP))
    shared_inner = (jax.nn.silu(shared_gate) * shared_up).astype(jnp.bfloat16)
    mixture = routed + project(shared_inner, sh_down)
    return layer_norm(res_scale * normed_mid.astype(jnp.float32) + mixture, norm2_gain).astype(jnp.bfloat16)
```

```python
import functools

import jax
import jax.numpy as jnp
from jax import lax
from jax.experimental import pallas as pl
from jax.experimental.pallas import tpu as pltpu
from jax.sharding import PartitionSpec as P

res_scale = 2.0**0.5
decay_tau = 16.0
norm_eps = 1e-05
AHEAD = 10
F32 = jnp.float32
BF16 = jnp.bfloat16


def dot(left, right):
    return jnp.dot(left, right, preferred_element_type=F32)


def dot_nt(left, right):
    return lax.dot_general(left, right, (((1,), (1,)), ((), ())), preferred_element_type=F32)


def iota(shape, dim):
    return lax.broadcasted_iota(jnp.int32, shape, dim)


def iota_f(shape, dim):
    return iota(shape, dim).astype(F32)


def quotient(values, divisor):
    return jnp.floor((values + 0.5) * (1.0 / divisor))


def ones_where(mask):
    return jnp.where(mask, 1.0, 0.0)


def silu(x):
    return x * (1.0 / (1.0 + jnp.exp(-x)))


def pad_to(n, multiple):
    return -(-n // multiple) * multiple


def bands(count, per):
    return [(e * per // 8 * 8, pad_to((e + 1) * per, 8)) for e in range(count)]


def join_bands(pieces, per):
    spans = bands(len(pieces), per)
    tiles = []
    for row in range(0, spans[-1][1], 8):
        tile = None
        for e, (first, last) in enumerate(spans):
            if first <= row < last:
                part = pieces[e][row - first : row - first + 8]
                if tile is None:
                    tile = part
                else:
                    tile = jnp.where(iota((8, 1), 0) + row < e * per, tile, part)
        tiles.append(tile)
    return jnp.concatenate(tiles, 0)


def kernel(dims, *refs):
    (rows, heads, kdim, vdim, width, cols, tp, ep, local, cap, top, ff, fs, chunks, nch, r16) = dims
    (tok_h, dd_h, du_h, db_h, hg_h, g1_h, ids_h, rw_h, g2_h) = refs[0:9]
    (state_h, wq_h, wk_h, wv_h, wg_h, wo_h, eg_h, eu_h, ed_h, sg_h, su_h, sd_h) = refs[9:21]
    out = refs[21]
    (tok_v, dd_v, du_v, db_v, hg_v, g1_v, ids_v, rw_v, g2_v) = refs[22:31]
    (state, wq, wk, wv, wg, wo, eg, eu, ed, sg, su, sd) = refs[31:43]
    (dq_ref, att_ref, head_out, val_s, route_s, route_r, pick, give_hi, give_lo) = refs[43:52]
    (p1s, p1r, sum_s, sum_r, sq_s, sq_r, ln_s, ln_r, inv_s, inv_r, xs, xr) = refs[52:64]
    (es, er, eo, ys, yr, inner) = refs[64:70]
    (hs, hr, ho, hys, hyr, hinner) = refs[70:76]
    (bs, br) = refs[76:78]
    (load_sem, tp_send, tp_recv, ep_send, ep_recv) = refs[78:83]

    experts = local * ep
    ny = tp // 2
    ns = ep // nch
    per = ns * cap
    slots = local * per
    lanes = ns * rows
    hf, hfs = ff // 2, fs // 2
    me_t = lax.axis_index("tp")
    me_e = lax.axis_index("ep")
    me_c = lax.rem(me_t, 2)

    def tp_peer(i, f):
        return lax.rem(me_t - me_c + 2 * i, tp) + me_c + f * (1 - 2 * me_c)

    def ep_peer(offset):
        return lax.rem(me_e + offset, ep)

    barrier = pltpu.get_barrier_semaphore()
    loads = []

    def add_load(src, dst):
        loads.append(pltpu.make_async_copy(src, dst, load_sem.at[len(loads)]))
        return len(loads) - 1

    i_tok = add_load(tok_h, tok_v)
    i_dd = add_load(dd_h, dd_v)
    i_wq = add_load(wq_h, wq)
    i_small = [
        add_load(src, dst)
        for src, dst in zip(
            (du_h, db_h, ids_h, rw_h, hg_h, g1_h, g2_h),
            (du_v, db_v, ids_v, rw_v, hg_v, g1_v, g2_v),
        )
    ]
    i_wk = add_load(wk_h, wk)
    step = rows // chunks
    i_state = [
        add_load(state_h.at[pl.ds(c * step, step)], state.at[pl.ds(c * step, step)])
        for c in range(chunks)
    ]
    half = wv_h.shape[0] // 2
    i_wv = [add_load(wv_h.at[pl.ds(c * half, half)], wv.at[pl.ds(c * half, half)]) for c in range(2)]
    i_wg = [add_load(wg_h.at[pl.ds(c * half, half)], wg.at[pl.ds(c * half, half)]) for c in range(2)]
    tp_order = [(i, f) for i in range(1, ny) for f in range(2)] + [(0, 1), (0, 0)]
    i_wo = []
    for n, (i, f) in enumerate(tp_order):
        start = pl.multiple_of(tp_peer(i, f) * cols, 128)
        i_wo.append(add_load(wo_h.at[:, pl.ds(start, cols)], wo.at[n]))
    i_sg = add_load(sg_h, sg)
    i_su = add_load(su_h, su)
    i_eg = add_load(eg_h, eg)
    i_eu = add_load(eu_h, eu)
    i_sd = add_load(sd_h, sd)
    i_ed = add_load(ed_h, ed)
    ahead = AHEAD + 10
    for copy in loads[:ahead]:
        copy.start()

    def ready(index):
        loads[index].wait()
        if index + ahead < len(loads):
            loads[index + ahead].start()

    for i, f in tp_order[:-1]:
        pl.semaphore_signal(
            barrier, inc=1, device_id=(me_e, tp_peer(i, f)), device_id_type=pl.DeviceIdType.MESH
        )
    for offset in range(1, ep):
        pl.semaphore_signal(
            barrier, inc=1, device_id=(ep_peer(offset), me_t), device_id_type=pl.DeviceIdType.MESH
        )

    sent = []

    def tp_copy(src, dst, kind, i, f):
        return pltpu.make_async_remote_copy(
            src_ref=src,
            dst_ref=dst,
            send_sem=tp_send.at[kind, 2 * i + f],
            recv_sem=tp_recv.at[kind, 2 * i + f],
            device_id=(me_e, tp_peer(i, f)),
            device_id_type=pl.DeviceIdType.MESH,
        )

    def tp_start(src, dst, kind, i, f):
        copy = tp_copy(src, dst, kind, i, f)
        copy.start()
        sent.append(copy)
        return copy

    def ep_start(src, dst, kind, slot, offset):
        copy = pltpu.make_async_remote_copy(
            src_ref=src,
            dst_ref=dst,
            send_sem=ep_send.at[kind, slot],
            recv_sem=ep_recv.at[kind, slot],
            device_id=(ep_peer(offset), me_t),
            device_id_type=pl.DeviceIdType.MESH,
        )
        copy.start()
        sent.append(copy)
        return copy

    def to_row(col, spread, shift):
        mask = iota((rows, spread), 1) == iota((rows, spread), 0) + shift
        return jnp.sum(jnp.where(mask, col, 0.0), 0, keepdims=True)

    def to_col(row):
        mask = iota((rows, row.shape[1]), 1) == iota((rows, row.shape[1]), 0)
        return jnp.sum(jnp.where(mask, row, 0.0), 1, keepdims=True)

    ready(i_tok)
    ready(i_dd)
    tok = tok_v[...]
    decay_low = dot_nt(tok, dd_v[...]).astype(BF16)
    ready(i_wq)
    queries = dot(tok, wq[...]).astype(BF16).astype(F32) * kdim ** (-0.5)
    for i in i_small:
        ready(i)
    pre = dot(decay_low, du_v[...]) + db_v[...]
    log_decay = (jnp.minimum(pre, 0.0) - jnp.log(1.0 + jnp.exp(-jnp.abs(pre)))) * (1.0 / decay_tau)
    dq_ref[...] = queries * jnp.exp(log_decay)

    ids = ids_v[...]
    weights = rw_v[...]
    line = iota_f((ep * r16, rows), 0)
    line_dev = quotient(line, r16)
    line_in = line - line_dev * r16
    line_kind = quotient(line_in, local)
    line_expert = (line_dev * local + line_in - line_kind * local).astype(jnp.int32)
    member = jnp.zeros((ep * r16, rows), F32)
    weight_of = jnp.zeros((ep * r16, rows), F32)
    for k in range(top):
        hit = ids[k : k + 1, :] == line_expert
        member = jnp.where(hit, 1.0, member)
        weight_of = jnp.where(hit, weights[k : k + 1, :], weight_of)
    earlier = ones_where(iota((rows, rows), 0) < iota((rows, rows), 1)).astype(BF16)
    rank = dot(member.astype(BF16), earlier)
    weight_hi = weight_of.astype(BF16).astype(F32)
    packed = jnp.where(line_kind == 0.0, member * (rank + 1.0), 0.0)
    packed = jnp.where(line_kind == 1.0, weight_hi, packed)
    packed = jnp.where(line_kind == 2.0, weight_of - weight_hi, packed)
    val_s[...] = packed.reshape(ep, r16, rows)
    spread_w = route_s.shape[2]
    for offset in range(ep):
        shift = offset // nch * rows
        spread = ones_where(iota((rows, spread_w), 1) == iota((rows, spread_w), 0) + shift)
        route_s[offset] = dot(val_s[ep_peer(offset)].astype(BF16), spread.astype(BF16)).astype(BF16)

    ready(i_wk)
    key_rows = dot(tok, wk[...]).astype(BF16).astype(F32)
    pairs = queries * key_rows
    key_width = heads * kdim
    hr_pad = att_ref.shape[1]
    head_mask = quotient(iota_f((hr_pad, key_width), 1), kdim) == iota_f((hr_pad, key_width), 0)
    far_first = sorted(range(1, ep), key=lambda o: (o % nch, -min(o, ep - o)))
    route_copies = []
    for c in range(chunks):
        ready(i_state[c])

        def one_row(b, carry):
            left = jnp.where(head_mask, dq_ref[pl.ds(b, 1), :], 0.0).astype(BF16)
            right = state[b].reshape(key_width, vdim).astype(BF16)
            att_ref[b] = dot(left, right)
            return carry

        lax.fori_loop(c * step, (c + 1) * step, one_row, 0, unroll=min(step, 3))
        if c == 0:
            pl.semaphore_wait(barrier, tp - 1 + ep - 1)
            route_r[0] = route_s[0]
            for offset in far_first:
                route_copies.append(
                    ep_start(route_s.at[offset], route_r.at[offset], 0, offset, offset)
                )
    for i in i_wv:
        ready(i)
    values = dot(tok, wv[...]).astype(BF16).astype(F32)
    for i in i_wg:
        ready(i)
    gate_pre = dot(tok, wg[...]).astype(BF16).astype(F32)
    for h in range(heads):
        part = slice(h * vdim, (h + 1) * vdim)
        score = jnp.sum(pairs[:, h * kdim : (h + 1) * kdim], -1, keepdims=True)
        attended = att_ref[:, h, :] + score * values[:, part]
        inv = lax.rsqrt(jnp.mean(attended * attended, -1, keepdims=True) + norm_eps)
        head_out[:, part] = (attended * inv * hg_v[...] * silu(gate_pre[:, part])).astype(BF16)

    heads_side = head_out[...]
    own, total_cols = None, None
    for n, (i, f) in enumerate(tp_order):
        ready(i_wo[n])
        product = dot(heads_side, wo[n])
        if (i, f) == (0, 0):
            own = product
        else:
            rounded = product.astype(BF16)
            p1s[n] = rounded
            tp_start(p1s.at[n], p1r.at[n], 0, i, f)
            product = rounded.astype(F32)
        total_cols = product if total_cols is None else total_cols + product
    row_sum = to_row(jnp.sum(total_cols, -1, keepdims=True), sum_s.shape[1], 0)
    sum_s[...] = jnp.broadcast_to(row_sum, sum_s.shape)
    for n, (i, f) in enumerate(tp_order[:-1]):
        tp_start(sum_s, sum_r.at[n], 1, i, f)

    for copy in route_copies:
        copy.wait_recv()
    slot_f = iota_f((slots, lanes), 0)
    slot_expert = quotient(slot_f, per)
    slot_in = slot_f - slot_expert * per
    slot_source = quotient(slot_in, cap)
    slot_code = slot_in - slot_source * cap + 1.0
    same_source = quotient(iota_f((slots, lanes), 1), rows) == slot_source
    eye = ones_where(iota((lanes, lanes), 0) == iota((lanes, lanes), 1)).astype(BF16)
    for p in range(nch):
        table = route_r[p].astype(F32)
        for q in range(1, ns):
            table = table + route_r[q * nch + p].astype(F32)
        table = table[:, 0:lanes]

        def rows_of(kind):
            spread = jnp.zeros((slots, lanes), F32)
            for k in range(local):
                line_at = kind * local + k
                spread = jnp.where(slot_expert == k, table[line_at : line_at + 1, :], spread)
            return spread

        placed = (rows_of(0) == slot_code) & same_source
        pick[p] = ones_where(placed).astype(BF16)
        give_hi[p] = dot_nt(eye, jnp.where(placed, rows_of(1), 0.0).astype(BF16)).astype(BF16)
        give_lo[p] = dot_nt(eye, jnp.where(placed, rows_of(2), 0.0).astype(BF16)).astype(BF16)

    start = pl.multiple_of(me_t * cols, 128)
    resid = own + res_scale * tok_v[:, pl.ds(start, cols)].astype(F32)
    token_sum = res_scale * jnp.sum(tok.astype(F32), -1, keepdims=True)
    for n, (i, f) in enumerate(tp_order[:-1]):
        tp_copy(p1s.at[n], p1r.at[n], 0, i, f).wait_recv()
        resid = resid + p1r[n].astype(F32)
    for n, (i, f) in enumerate(tp_order[:-1]):
        tp_copy(sum_s, sum_r.at[n], 1, i, f).wait_recv()
        row_sum = row_sum + sum_r[n][0:1, :]
    mean = (to_col(row_sum) + token_sum) * (1.0 / width)
    center = resid - mean
    gained = center * g1_v[...]
    xs[...] = gained.astype(BF16)
    x_copies = {}
    for offset in far_first:
        x_copies[offset] = ep_start(xs, xr.at[offset % nch, offset // nch], 1, offset, offset)
    xr[0, 0] = xs[...]
    squares = to_row(jnp.sum(center * center, -1, keepdims=True), sq_s.shape[1], 0)
    sq_s[...] = jnp.broadcast_to(squares, sq_s.shape)
    for n, (i, f) in enumerate(tp_order[:-1]):
        tp_start(sq_s, sq_r.at[n], 2, i, f)
    for n, (i, f) in enumerate(tp_order[:-1]):
        tp_copy(sq_s, sq_r.at[n], 2, i, f).wait_recv()
        squares = squares + sq_r[n][0:1, :]
    inv_col = to_col(lax.rsqrt(squares * (1.0 / width) + norm_eps))
    for q in range(ns):
        inv_s[q] = jnp.broadcast_to(to_row(inv_col, inv_s.shape[2], q * rows), inv_s.shape[1:])
    inv_copies = {}
    for offset in far_first:
        inv_copies[offset] = ep_start(
            inv_s.at[offset // nch], inv_r.at[offset], 2, offset, offset
        )
    inv_r[0] = inv_s[0]
    normed = (gained * inv_col).astype(BF16)

    def first_step(product, s_ref, r_ref, o_ref, kind, h):
        s_ref[...] = product(pl.multiple_of((1 - me_c) * h, 128)).astype(BF16)
        tp_start(s_ref, r_ref, kind, 0, 1)
        o_ref[...] = product(pl.multiple_of(me_c * h, 128))

    def second_step(s_ref, r_ref, o_ref, ys_ref, yr_ref, kind):
        tp_copy(s_ref, r_ref, kind, 0, 1).wait_recv()
        total = o_ref[...] + r_ref[...].astype(F32)
        o_ref[...] = total
        ys_ref[...] = total.astype(BF16)
        for i in range(1, ny):
            tp_start(ys_ref, yr_ref.at[i], kind + 1, i, 0)

    def third_step(o_ref, ys_ref, yr_ref, in_ref, kind, h, scale):
        total = o_ref[...]
        for i in range(1, ny):
            tp_copy(ys_ref, yr_ref.at[i], kind + 1, i, 0).wait_recv()
            total = total + yr_ref[i].astype(F32)
        if scale is not None:
            total = total * scale
        in_ref[me_c] = (silu(total[:, 0:h]) * total[:, h : 2 * h]).astype(BF16)
        tp_start(in_ref.at[me_c], in_ref.at[me_c], kind + 2, 0, 1)

    def fourth_step(in_ref, kind):
        sib = 1 - me_c
        tp_copy(in_ref.at[sib], in_ref.at[sib], kind + 2, 0, 1).wait_recv()

    ready(i_sg)
    ready(i_su)

    def shared_half(at):
        gate = dot(normed, sg[:, pl.ds(at, hfs)])
        return jnp.concatenate([gate, dot(normed, su[:, pl.ds(at, hfs)])], 1)

    first_step(shared_half, hs, hr, ho, 4, hfs)

    def routed_first(p):
        chosen = dot(pick[p], xr[p].reshape(lanes, cols))
        parts = [chosen[a:b].astype(BF16) for a, b in bands(local, per)]

        def routed_half(at):
            return join_bands(
                [
                    jnp.concatenate(
                        [
                            dot(parts[e], eg[e, :, pl.ds(at, hf)]),
                            dot(parts[e], eu[e, :, pl.ds(at, hf)]),
                        ],
                        1,
                    )
                    for e in range(local)
                ],
                per,
            )

        first_step(routed_half, es.at[p], er.at[p], eo.at[p], 7 + 3 * p, hf)

    def routed_third(p):
        for offset in range(p, ep, nch):
            if offset:
                inv_copies[offset].wait_recv()
        inv = inv_r[p][0:1, 0:lanes]
        for q in range(1, ns):
            inv = inv + inv_r[q * nch + p][0:1, 0:lanes]
        scale = jnp.sum(pick[p].astype(F32) * inv, -1, keepdims=True)
        third_step(eo.at[p], ys.at[p], yr.at[p], inner.at[p], 7 + 3 * p, hf, scale)

    back_copies = {}

    def routed_back(p):
        fourth_step(inner.at[p], 7 + 3 * p)
        low, high = inner[p, 0].astype(F32), inner[p, 1].astype(F32)
        answer = join_bands(
            [
                dot(low[a:b].astype(BF16), ed[e, 0:hf, :])
                + dot(high[a:b].astype(BF16), ed[e, hf:ff, :])
                for e, (a, b) in enumerate(bands(local, per))
            ],
            per,
        ).astype(BF16)
        returned = dot(give_hi[p], answer) + dot(give_lo[p], answer)
        bs[p] = returned.astype(BF16).reshape(ns, rows, cols)
        for offset in [o for o in far_first if o % nch == p]:
            back_copies[offset] = ep_start(
                bs.at[p, offset // nch], br.at[offset], 3, offset, ep - offset
            )

    ready(i_eg)
    ready(i_eu)
    for p in range(nch):
        for offset in range(p, ep, nch):
            if offset:
                x_copies[offset].wait_recv()
        routed_first(p)
        if p == 0:
            second_step(hs, hr, ho, hys, hyr, 4)
        else:
            third_step(ho, hys, hyr, hinner, 4, hfs, None)
        second_step(es.at[p], er.at[p], eo.at[p], ys.at[p], yr.at[p], 7 + 3 * p)
    if nch == 1:
        third_step(ho, hys, hyr, hinner, 4, hfs, None)
    ready(i_sd)
    ready(i_ed)
    for p in range(nch):
        routed_third(p)
        if p == nch - 1:
            fourth_step(hinner, 4)
            mixture = dot(hinner[0], sd[0:hfs, :]) + dot(hinner[1], sd[hfs:fs, :])
        routed_back(p)
    last = res_scale * normed.astype(F32) + mixture + bs[0, 0].astype(F32)
    for offset in [o for o in far_first[::-1] if o % nch == 0] + [o for o in far_first if o % nch]:
        back_copies[offset].wait_recv()
        last = last + br[offset].astype(F32)

    mean = jnp.mean(last, -1, keepdims=True)
    center = last - mean
    moment = jnp.sum(center * center, -1, keepdims=True)
    spread_r = ln_s.shape[1]
    mean_row = to_row(mean, spread_r, 0)
    moment_row = to_row(moment, spread_r, 0)
    ln_s[...] = jnp.where(iota((8, spread_r), 0) == 0, mean_row, moment_row)
    for n, (i, f) in enumerate(tp_order[:-1]):
        tp_start(ln_s, ln_r.at[n], 3, i, f)
    means = [mean_row]
    for n, (i, f) in enumerate(tp_order[:-1]):
        tp_copy(ln_s, ln_r.at[n], 3, i, f).wait_recv()
        tile = ln_r[n]
        means.append(tile[0:1, :])
        moment_row = moment_row + tile[1:2, :]
    total = sum(means) * (1.0 / tp)
    for m in means:
        moment_row = moment_row + cols * (m - total) * (m - total)
    scale = lax.rsqrt(moment_row * (1.0 / width) + norm_eps)
    out[...] = ((last - to_col(total)) * to_col(scale) * g2_v[...]).astype(BF16)
    for copy in sent:
        copy.wait_send()


def per_device(
    tokens,
    state,
    w_query,
    w_key,
    w_value,
    w_outgate,
    decay_down,
    decay_up,
    decay_bias,
    head_gain,
    w_output,
    norm1_gain,
    route_ids,
    route_weight,
    exp_gate,
    exp_up,
    exp_down,
    sh_gate,
    sh_up,
    sh_down,
    norm2_gain,
):
    rows, width = tokens.shape
    heads, kdim, vdim = state.shape[1:]
    tp, ep = lax.axis_size("tp"), lax.axis_size("ep")
    cols = width // tp
    top = route_ids.shape[1]
    local = exp_gate.shape[0]
    cap = max(2, rows * top // (local * ep) + 1)
    ff, fs = exp_gate.shape[2], sh_gate.shape[1]
    nch = 2 if ep % 2 == 0 else 1
    ns, ny = ep // nch, tp // 2
    slots = local * ns * cap
    lanes, lanes_pad = ns * rows, pad_to(ns * rows, 128)
    rows_pad = pad_to(rows, 128)
    r16 = pad_to(3 * local, 16)
    chunks = 4
    dims = (rows, heads, kdim, vdim, width, cols, tp, ep, local, cap, top, ff, fs, chunks, nch, r16)
    n_loads = 10 + 1 + chunks + 4 + tp + 6
    vm = pltpu.VMEM
    smalls = (
        tokens,
        decay_down.T,
        decay_up,
        decay_bias[None, :],
        head_gain[None, :],
        norm1_gain[None, :],
        route_ids.T,
        route_weight.T,
        norm2_gain[None, :],
    )
    return pl.pallas_call(
        functools.partial(kernel, dims),
        out_shape=pltpu.VMEM((rows, cols), BF16),
        in_specs=[pl.BlockSpec(memory_space=pl.ANY)] * 21,
        out_specs=pl.BlockSpec(memory_space=pltpu.VMEM),
        scratch_shapes=[vm(a.shape, a.dtype) for a in smalls]
        + [
            vm(state.shape, F32),
            vm(w_query.shape, BF16),
            vm(w_key.shape, BF16),
            vm(w_value.shape, BF16),
            vm(w_outgate.shape, BF16),
            vm((tp, w_output.shape[0], cols), BF16),
            vm(exp_gate.shape, BF16),
            vm(exp_up.shape, BF16),
            vm(exp_down.shape, BF16),
            vm(sh_gate.shape, BF16),
            vm(sh_up.shape, BF16),
            vm(sh_down.shape, BF16),
            vm((rows, heads * kdim), F32),
            vm((rows, pad_to(heads, 8), vdim), F32),
            vm((rows, heads * vdim), BF16),
            vm((ep, r16, rows), F32),
            vm((ep, r16, lanes_pad), BF16),
            vm((ep, r16, lanes_pad), BF16),
            vm((nch, slots, lanes), BF16),
            vm((nch, lanes, slots), BF16),
            vm((nch, lanes, slots), BF16),
            vm((tp, rows, cols), BF16),
            vm((tp, rows, cols), BF16),
            vm((8, rows_pad), F32),
            vm((tp, 8, rows_pad), F32),
            vm((8, rows_pad), F32),
            vm((tp, 8, rows_pad), F32),
            vm((8, rows_pad), F32),
            vm((tp, 8, rows_pad), F32),
            vm((ns, 8, lanes_pad), F32),
            vm((ep, 8, lanes_pad), F32),
            vm((rows, cols), BF16),
            vm((nch, ns, rows, cols), BF16),
            vm((nch, slots, ff), BF16),
            vm((nch, slots, ff), BF16),
            vm((nch, slots, ff), F32),
            vm((nch, slots, ff), BF16),
            vm((nch, ny, slots, ff), BF16),
            vm((nch, 2, slots, ff // 2), BF16),
            vm((rows, fs), BF16),
            vm((rows, fs), BF16),
            vm((rows, fs), F32),
            vm((rows, fs), BF16),
            vm((ny, rows, fs), BF16),
            vm((2, rows, fs // 2), BF16),
            vm((nch, ns, rows, cols), BF16),
            vm((ep, rows, cols), BF16),
            pltpu.SemaphoreType.DMA((n_loads,)),
            pltpu.SemaphoreType.DMA((13, tp)),
            pltpu.SemaphoreType.DMA((13, tp)),
            pltpu.SemaphoreType.DMA((4, ep)),
            pltpu.SemaphoreType.DMA((4, ep)),
        ],
        compiler_params=pltpu.CompilerParams(
            collective_id=0, has_side_effects=True, vmem_limit_bytes=60 * 1024 * 1024
        ),
        name="layer",
    )(
        *smalls,
        state,
        w_query,
        w_key,
        w_value,
        w_outgate,
        w_output,
        exp_gate,
        exp_up,
        exp_down,
        sh_gate,
        sh_up,
        sh_down,
    )


def solution(mesh):
    in_specs = (
        P("ep", None),
        P("ep", "tp", None, None),
        P(None, "tp"),
        P(None, "tp"),
        P(None, "tp"),
        P(None, "tp"),
        P(),
        P(None, "tp"),
        P("tp"),
        P(),
        P("tp", None),
        P("tp"),
        P("ep", None),
        P("ep", None),
        P("ep", "tp", None),
        P("ep", "tp", None),
        P("ep", None, "tp"),
        P("tp", None),
        P("tp", None),
        P(None, "tp"),
        P("tp"),
    )
    out_specs = P("ep", "tp")
    return jax.shard_map(
        per_device, mesh=mesh, in_specs=in_specs, out_specs=out_specs, check_vma=False
    )
```
